256 devices in a mesh: grp: 2 (over y), ep: 64 (over z, x), tp: 2 (over core).
Axes of the slice: x: 4, y: 2, z: 16, core: 2. Of those that a mesh axis runs over, the one named last changes fastest.
The devices are a block of a 4x16x16 slice.
Arguments:
- fresh_inputs: bfloat16 [2048, 2048], P(('grp', 'ep')), parts along dimension 0, may hold values from -6 to 6
- memory_arrays: float32 [2048, 32, 64, 64], P(('grp', 'ep'), 'tp'), parts along dimension 0, may hold values from -4 to 4
- chosen_specialist: int32 [2048, 2], P(('grp', 'ep')), parts along dimension 0, may hold values from 0 to 3, all different within a row; in each aligned block of 1024 rows (0 to 1023, 1024 to 2047, ...) at most 768 rows name the same one
- chosen_coefficient: bfloat16 [2048, 2], P(('grp', 'ep')), parts along dimension 0, may hold values from 0.25 to 1
- first_rescale: float32 [2048], replicated, may hold values from 0.1 to 1.9
- second_rescale: float32 [2048], replicated, may hold values from 0.1 to 1.9
- receiver_projector: bfloat16 [2048, 2048], P('tp', 'ep'), may hold values from -0.125 to 0.125
- address_projector: bfloat16 [2048, 2048], P('tp', 'ep'), may hold values from -0.125 to 0.125
- content_projector: bfloat16 [2048, 2048], P('tp', 'ep'), may hold values from -0.125 to 0.125
- final_projector: bfloat16 [2048, 2048], P('tp', 'ep'), may hold values from -0.125 to 0.125
- forget_narrowing: bfloat16 [2048, 64], replicated, may hold values from -0.125 to 0.125
- forget_widening: bfloat16 [64, 2048], P(None, 'tp'), may hold values from -0.75 to 0.75
- forget_bias: float32 [2048], P('tp'), may hold values from -3 to 1
- learning_narrowing: bfloat16 [2048, 64], replicated, may hold values from -0.125 to 0.125
- learning_widening: bfloat16 [64, 2048], P(None, 'tp'), may hold values from -0.75 to 0.75
- learning_bias: float32 [2048], P('tp'), may hold values from -1.5 to 1.5
- lane_scaling: float32 [2048], P('tp'), may hold values from 0.1 to 1.9
- instant_reward: float32 [32, 64], P('tp'), may hold values from -0.5 to 0.5
- specialist_switch: bfloat16 [2048, 28672], P(None, ('ep', 'tp')), may hold values from -0.125 to 0.125
- specialist_expand: bfloat16 [2048, 28672], P(None, ('ep', 'tp')), may hold values from -0.125 to 0.125
- specialist_contract: bfloat16 [28672, 2048], P(('ep', 'tp')), may hold values from -0.0625 to 0.0625
- common_activator: bfloat16 [2048, 5632], P(None, ('ep', 'tp')), may hold values from -0.125 to 0.125
- common_expand: bfloat16 [2048, 5632], P(None, ('ep', 'tp')), may hold values from -0.125 to 0.125
- common_contract: bfloat16 [5632, 2048], P(('ep', 'tp')), may hold values from -0.078125 to 0.078125
- common_switch: bfloat16 [2048], replicated, may hold values from -0.125 to 0.125
Outputs:
- new_tokens: bfloat16 [2048, 2048], P(('grp', 'ep', 'tp')), parts along dimension 0
- memory_after: float32 [2048, 32, 64, 64], P(('grp', 'ep'), 'tp'), parts along dimension 0
The draws below stay inside these ranges and needn't reach their ends.
There are 2 independent parts, one for each index of `grp`. The reference program is written for one: setup_inputs(seed, part) draws one part's arguments, and reference() takes and returns one part's arrays. A program takes and returns all parts, laid end to end along the dimension named above; an argument that names none is the same for every part. Nothing has to cross between parts.
Inputs may be any that keep to these rules, and one draw needn't show every extreme that they name: `chosen_specialist`: each row names 2 different experts. Over the whole batch no expert is named by more than 768 rows, and in every draw some expert is named by exactly 768 rows.
All inputs are finite; a program needn't handle non-finite values.
Results may differ from the reference program's by a relative error of at most 0.014.
Values may be sent and summed in bfloat16 or wider, within the bound.
No kernel may reach another device: no remote copies, remote signals or barrier semaphores. Data moves between devices by JAX's collectives and lax.ppermute only.
A program may use at most 128 MiB of HBM per device.

```python
import math
import jax
import jax.numpy as jnp
import numpy as np
from jax import lax

MODEL_DIM = 2048
LANE_WIDTH = 64
LANE_COUNT = 32
LOWRANK_DIM = 64
EXPERTS = 4
TOP_K = 2
FF_E = 7168
DENSE_FF = 5632
BATCH = 1024
CAP = 768
N_TP = 2


def block_levels(rng, shape, pieces, low, largest):
    level, own = 1.0, jax.random.fold_in(rng, 6)
    for dim, parts in pieces:
        steps = jnp.exp(jax.random.uniform(jax.random.fold_in(own, dim), (parts,), jnp.float32, low / len(pieces), largest / len(pieces)))
        level = level * jnp.repeat(steps, shape[dim] // parts).reshape([-1 if axis == dim else 1 for axis in range(len(shape))])
    return level


def assign_block(stream_key, own, number, rows, amount, top, most, lean):
    ranking = jax.random.permutation(stream_key, amount)
    packed, common = shares(amount, rows * top, most, lean, True), shares(amount, rows * top, most, lean, False)
    places = jnp.arange(amount)

    def named(tallies, offset_by):
        used = int((tallies > 0).sum())
        fixed = max(1, used // 4)
        moved = fixed + (places - fixed + offset_by * (used - fixed)) % max(1, amount - fixed)
        return jnp.zeros((amount,), jnp.int32).at[ranking[jnp.where(places < fixed, places, moved)]].set(jnp.asarray(tallies, jnp.int32))

    tallies = jnp.where(number % 4 == 0, named(packed, number // 4), named(common, number - number // 4 - 1))
    mixed = jax.random.permutation(jax.random.fold_in(own, 3), amount)
    source_of, sink = mixed[0:amount // 2 * 2:2], mixed[1:amount // 2 * 2:2]
    slack = jnp.minimum(tallies[source_of] - 1, most - tallies[sink]) // 2
    slack = jnp.where((source_of == ranking[0]) | (sink == ranking[0]) | (tallies[sink] == 0), 0, jnp.maximum(slack, 0))
    moved = jax.random.randint(jax.random.fold_in(own, 4), (amount // 2,), 0, 1 << 20) % (slack + 1)
    tallies = tallies.at[source_of].add(-moved).at[sink].add(moved)
    members = jnp.searchsorted(jnp.cumsum(tallies), jnp.arange(rows * top), side="right").astype(jnp.int32)
    listing = members.reshape(top, rows).T
    listing = listing[jax.random.permutation(jax.random.fold_in(own, 1), rows)]
    offset_by = jax.random.randint(jax.random.fold_in(own, 2), (rows, 1), 0, top)
    return jnp.take_along_axis(listing, (jnp.arange(top)[None, :] + offset_by) % top, axis=1)


def shares(count, total, reach, lean, full):
    portions = [(1 << 20) // math.isqrt(rank ** lean) + 1 for rank in range(1, count + 1)]
    largest = reach if full else min(reach, max(-(-total // count), total * portions[0] // sum(portions)))
    least = 1 if total - largest >= count - 1 else 0
    holding, surplus = [largest] + [least] * (count - 1), total - largest - least * (count - 1)
    while surplus > 0:
        free = [i for i in range(1, count) if holding[i] < largest] or [i for i in range(1, count) if holding[i] < reach]
        pool, remaining = sum([portions[i] for i in free]), surplus
        for i in free:
            addition = min(reach - holding[i], max(1, remaining * portions[i] // pool), surplus)
            holding[i] = holding[i] + addition
            surplus = surplus - addition
    return np.array(holding)


def bell_draw(rng, dims, deviation, limit, cuts=(), dtype=jnp.bfloat16):
    gain = block_levels(rng, dims, cuts, -0.22, 0.18) if cuts else 1.0
    drawn = jax.random.normal(rng, dims, jnp.float32) * deviation * gain
    return jnp.minimum(jnp.maximum(drawn, -limit), limit).astype(dtype)


def setup_inputs(seed: int = 0, part: int = 0) -> dict:
    splits = jax.random.split(jax.random.key(seed), 26)
    own_keys = jax.random.split(jax.random.fold_in(splits[25], part), 26)
    fresh_inputs = bell_draw(own_keys[0], (BATCH, MODEL_DIM), 1.0, 6.0, ((0, 64),))
    memory_arrays = bell_draw(own_keys[1], (BATCH, LANE_COUNT, LANE_WIDTH, LANE_WIDTH), 0.5, 4.0, ((0, 64), (1, 2)), jnp.float32)
    chosen_specialist_keys = jax.random.split(jax.random.fold_in(own_keys[2], 1), BATCH // BATCH)
    chosen_specialist_turns = jax.random.permutation(jax.random.fold_in(own_keys[2], 3), BATCH // BATCH)
    chosen_specialist = jax.vmap(lambda own, number: assign_block(jax.random.fold_in(own_keys[2], 2), own, number, BATCH, EXPERTS, TOP_K, CAP, 2))(chosen_specialist_keys, chosen_specialist_turns).reshape((BATCH, TOP_K))
    chosen_coefficient = jnp.clip(0.25 + 0.75 * jax.random.uniform(own_keys[3], (BATCH, TOP_K), jnp.float32) ** block_levels(own_keys[3], (BATCH, TOP_K), ((0, 64),), -0.2, 0.2), 0.25, 1.0).astype(jnp.bfloat16)
    first_rescale = jnp.clip(1.0 + 0.18 * jax.random.normal(splits[4], (MODEL_DIM,), jnp.float32), 0.1, 1.9)
    second_rescale = jnp.clip(1.0 + 0.18 * jax.random.normal(splits[5], (MODEL_DIM,), jnp.float32), 0.1, 1.9)
    receiver_projector = bell_draw(splits[6], (MODEL_DIM, MODEL_DIM), MODEL_DIM ** -0.5, 0.125, ((0, 2), (1, 64)))
    address_projector = bell_draw(splits[7], (MODEL_DIM, MODEL_DIM), MODEL_DIM ** -0.5, 0.125, ((0, 2), (1, 64)))
    content_projector = bell_draw(splits[8], (MODEL_DIM, MODEL_DIM), MODEL_DIM ** -0.5, 0.125, ((0, 2), (1, 64)))
    final_projector = bell_draw(splits[9], (MODEL_DIM, MODEL_DIM), MODEL_DIM ** -0.5, 0.125, ((0, 2), (1, 64)))
    forget_narrowing = bell_draw(splits[10], (MODEL_DIM, LOWRANK_DIM), MODEL_DIM ** -0.5, 0.125)
    forget_widening = bell_draw(splits[11], (LOWRANK_DIM, MODEL_DIM), LOWRANK_DIM ** -0.5, 0.75, ((1, 2),))
    forget_bias = jnp.clip(-3.0 + 4.0 * jax.random.uniform(splits[12], (MODEL_DIM,), jnp.float32) ** block_levels(splits[12], (MODEL_DIM,), ((0, 2),), -0.2, 0.2), -3.0, 1.0)
    learning_narrowing = bell_draw(splits[13], (MODEL_DIM, LOWRANK_DIM), MODEL_DIM ** -0.5, 0.125)
    learning_widening = bell_draw(splits[14], (LOWRANK_DIM, MODEL_DIM), LOWRANK_DIM ** -0.5, 0.75, ((1, 2),))
    learning_bias = jnp.clip(jax.random.uniform(splits[15], (MODEL_DIM,), jnp.float32, -1.5, 1.5) * block_levels(splits[15], (MODEL_DIM,), ((0, 2),), -0.4, 0.0), -1.5, 1.5)
    lane_scaling = jnp.clip(1.0 + 0.18 * jax.random.normal(splits[16], (MODEL_DIM,), jnp.float32), 0.1, 1.9)
    instant_reward = bell_draw(splits[17], (LANE_COUNT, LANE_WIDTH), 0.1, 0.5, ((0, 2),), jnp.float32)
    specialist_switch = bell_draw(splits[18], (MODEL_DIM, EXPERTS * FF_E), MODEL_DIM ** -0.5, 0.125, ((1, 128),))
    specialist_expand = bell_draw(splits[19], (MODEL_DIM, EXPERTS * FF_E), MODEL_DIM ** -0.5, 0.125, ((1, 128),))
    specialist_contract = bell_draw(splits[20], (EXPERTS * FF_E, MODEL_DIM), FF_E ** -0.5, 0.0625, ((0, 128),))
    common_activator = bell_draw(splits[21], (MODEL_DIM, DENSE_FF), MODEL_DIM ** -0.5, 0.125, ((1, 128),))
    common_expand = bell_draw(splits[22], (MODEL_DIM, DENSE_FF), MODEL_DIM ** -0.5, 0.125, ((1, 128),))
    common_contract = bell_draw(splits[23], (DENSE_FF, MODEL_DIM), DENSE_FF ** -0.5, 0.078125, ((0, 128),))
    common_switch = bell_draw(splits[24], (MODEL_DIM,), MODEL_DIM ** -0.5, 0.125)
    return dict(fresh_inputs=fresh_inputs, memory_arrays=memory_arrays, chosen_specialist=chosen_specialist, chosen_coefficient=chosen_coefficient, first_rescale=first_rescale, second_rescale=second_rescale, receiver_projector=receiver_projector, address_projector=address_projector, content_projector=content_projector, final_projector=final_projector, forget_narrowing=forget_narrowing, forget_widening=forget_widening, forget_bias=forget_bias, learning_narrowing=learning_narrowing, learning_widening=learning_widening, learning_bias=learning_bias, lane_scaling=lane_scaling, instant_reward=instant_reward, specialist_switch=specialist_switch, specialist_expand=specialist_expand, specialist_contract=specialist_contract, common_activator=common_activator, common_expand=common_expand, common_contract=common_contract, common_switch=common_switch)


RMS_EPS = 1e-06
GROUP_EPS = 0.00064
HIGHEST = lax.Precision.HIGHEST

def rms_norm(values, norm_gain):
    mean_sq = lax.optimization_barrier(jnp.mean(values * values, axis=-1, keepdims=True))
    return values * lax.rsqrt(mean_sq + RMS_EPS) * norm_gain

def split_product(left_rows, weight_rows):
    block_width = left_rows.shape[1] // N_TP
    running = jnp.zeros((left_rows.shape[0], weight_rows.shape[1]), jnp.float32)
    for block_index in range(N_TP):
        lower = block_index * block_width
        product = jnp.dot(left_rows[:, lower:lower + block_width], weight_rows[lower:lower + block_width], preferred_element_type=jnp.float32)
        running = running + lax.optimization_barrier(product.astype(jnp.bfloat16)).astype(jnp.float32)
    return running.astype(jnp.bfloat16)

def evolve_memory(memory_arrays, receiver_lanes, address_lanes, content_lanes, forget_lanes, learning_lanes, lane_rescale, instant_reward):
    unit_key = address_lanes * lax.rsqrt(lax.optimization_barrier(jnp.sum(address_lanes * address_lanes, axis=-1, keepdims=True)) + 1.0)
    stepped_address = address_lanes * learning_lanes
    removal = jnp.einsum('bhvk,bhk->bhv', memory_arrays, unit_key, precision=HIGHEST)
    memory_after = memory_arrays * forget_lanes[:, :, None, :] - removal[..., None] * (unit_key * learning_lanes)[:, :, None, :] + content_lanes[..., None] * stepped_address[:, :, None, :]
    memory_retrieval = jnp.einsum('bhvk,bhk->bhv', memory_after, receiver_lanes, precision=HIGHEST)
    centred = memory_retrieval - lax.optimization_barrier(jnp.mean(memory_retrieval, axis=-1, keepdims=True))
    unit_address = centred * lax.rsqrt(lax.optimization_barrier(jnp.mean(centred * centred, axis=-1, keepdims=True)) + GROUP_EPS)
    instant_extra = lax.optimization_barrier(jnp.sum(receiver_lanes * stepped_address * instant_reward, axis=-1, keepdims=True)) * content_lanes
    return (memory_after, unit_address * lane_rescale + instant_extra)

def swiglu(rows_in, gate_w, up_w):
    gate_val = jnp.dot(rows_in, gate_w, preferred_element_type=jnp.float32)
    up_val = jnp.dot(rows_in, up_w, preferred_element_type=jnp.float32)
    return (jax.nn.silu(gate_val) * up_val).astype(jnp.bfloat16)

def reference(fresh_inputs, memory_arrays, chosen_specialist, chosen_coefficient, first_rescale, second_rescale, receiver_projector, address_projector, content_projector, final_projector, forget_narrowing, forget_widening, forget_bias, learning_narrowing, learning_widening, learning_bias, lane_scaling, instant_reward, specialist_switch, specialist_expand, specialist_contract, common_activator, common_expand, common_contract, common_switch):
    batch_rows = fresh_inputs.shape[0]
    residual = fresh_inputs.astype(jnp.float32)
    normed = rms_norm(residual, first_rescale).astype(jnp.bfloat16)
    receiver_array = split_product(normed, receiver_projector)
    address_mapped = split_product(normed, address_projector)
    content_array = split_product(normed, content_projector)
    decay_mid = jnp.tanh(jnp.dot(normed, forget_narrowing, preferred_element_type=jnp.float32)).astype(jnp.bfloat16)
    decay_pre = forget_bias + jnp.dot(decay_mid, forget_widening, preferred_element_type=jnp.float32)
    forget_multiplier = jnp.exp(-jnp.exp(-jax.nn.softplus(-decay_pre) - 0.5))
    rate_mid = jnp.dot(normed, learning_narrowing, preferred_element_type=jnp.float32).astype(jnp.bfloat16)
    learning_step = jax.nn.sigmoid(learning_bias + jnp.dot(rate_mid, learning_widening, preferred_element_type=jnp.float32))

    def divide_lanes(channels):
        return channels.astype(jnp.float32).reshape(batch_rows, LANE_COUNT, LANE_WIDTH)
    memory_after, memory_retrieval = evolve_memory(memory_arrays, divide_lanes(receiver_array), divide_lanes(address_mapped), divide_lanes(content_array), divide_lanes(forget_multiplier), divide_lanes(learning_step), lane_scaling.reshape(LANE_COUNT, LANE_WIDTH), instant_reward)
    attended = memory_retrieval.reshape(batch_rows, MODEL_DIM).astype(jnp.bfloat16)
    mixed = split_product(attended, final_projector)
    residual = residual + mixed.astype(jnp.float32)
    ffn_in = rms_norm(residual, second_rescale).astype(jnp.bfloat16)
    routed = jnp.zeros((batch_rows, MODEL_DIM), jnp.float32)
    for expert in range(EXPERTS):
        lower = expert * FF_E
        hidden = swiglu(ffn_in, specialist_switch[:, lower:lower + FF_E], specialist_expand[:, lower:lower + FF_E])
        share = lax.optimization_barrier(jnp.sum(jnp.where(chosen_specialist == expert, chosen_coefficient.astype(jnp.float32), 0.0), axis=1))
        routed = routed + share[:, None] * jnp.dot(hidden, specialist_contract[lower:lower + FF_E], preferred_element_type=jnp.float32)
    shared_hidden = swiglu(ffn_in, common_activator, common_expand)
    branch_scale = jax.nn.sigmoid(jnp.dot(ffn_in, common_switch, preferred_element_type=jnp.float32))
    routed = routed + branch_scale[:, None] * jnp.dot(shared_hidden, common_contract, preferred_element_type=jnp.float32)
    return ((residual + routed).astype(jnp.bfloat16), memory_after)
```

```python
import jax
import jax.numpy as jnp
from jax import lax
from jax.sharding import Mesh
from jax.sharding import PartitionSpec as P


LANE_WIDTH = 64
FF_E = 7168
EP = ("ep_0", "ep_1")
GRP_EP = ("grp", "ep_0", "ep_1")
EP_TP = ("ep_0", "ep_1", "tp")
GRP_EP_TP = ("grp", "ep_0", "ep_1", "tp")


RMS_EPS = 1e-06
GROUP_EPS = 0.00064
HIGHEST = lax.Precision.HIGHEST
BF16 = jnp.bfloat16
F32 = jnp.float32


def from_ahead(value, axis, steps):
    size = lax.axis_size(axis)
    return lax.ppermute(value, axis, [((i + steps) % size, i) for i in range(size)])


def row_pieces(value, axis):
    return [value] + [from_ahead(value, axis, k) for k in range(1, lax.axis_size(axis))]


def in_row_order(pieces, axis):
    count = len(pieces)
    start = (count - lax.axis_index(axis)) % count
    twice = jnp.stack(pieces + pieces[:-1])
    return lax.dynamic_slice_in_dim(twice, start, count, 0)


def rms_norm(values, norm_gain):
    mean_sq = jnp.mean(values * values, axis=-1, keepdims=True)
    return values * lax.rsqrt(mean_sq + RMS_EPS) * norm_gain


def evolve_memory(
    memory_arrays,
    receiver_lanes,
    address_lanes,
    content_lanes,
    forget_lanes,
    learning_lanes,
    lane_rescale,
    instant_reward,
):
    unit_key = address_lanes * lax.rsqrt(
        jnp.sum(address_lanes * address_lanes, axis=-1, keepdims=True) + 1.0
    )
    stepped_address = address_lanes * learning_lanes
    removal = jnp.einsum("bhvk,bhk->bhv", memory_arrays, unit_key, precision=HIGHEST)
    memory_after = (
        memory_arrays * forget_lanes[:, :, None, :]
        - removal[..., None] * (unit_key * learning_lanes)[:, :, None, :]
        + content_lanes[..., None] * stepped_address[:, :, None, :]
    )
    memory_retrieval = jnp.einsum("bhvk,bhk->bhv", memory_after, receiver_lanes, precision=HIGHEST)
    centred = memory_retrieval - jnp.mean(memory_retrieval, axis=-1, keepdims=True)
    unit_address = centred * lax.rsqrt(
        jnp.mean(centred * centred, axis=-1, keepdims=True) + GROUP_EPS
    )
    instant_extra = (
        jnp.sum(receiver_lanes * stepped_address * instant_reward, axis=-1, keepdims=True)
        * content_lanes
    )
    return (memory_after, unit_address * lane_rescale + instant_extra)


def rows_dot(left, right_rows):
    return lax.dot_general(left, right_rows, (((1,), (1,)), ((), ())), preferred_element_type=F32)


def body(
    fresh_inputs,
    memory_arrays,
    chosen_specialist,
    chosen_coefficient,
    first_rescale,
    second_rescale,
    receiver_projector,
    address_projector,
    content_projector,
    final_projector,
    forget_narrowing,
    forget_widening,
    forget_bias,
    learning_narrowing,
    learning_widening,
    learning_bias,
    lane_scaling,
    instant_reward,
    specialist_switch,
    specialist_expand,
    specialist_contract,
    common_activator,
    common_expand,
    common_contract,
    common_switch,
):
    own_rows, model_width = fresh_inputs.shape
    tp_count = lax.axis_size("tp")
    tp_rank = lax.axis_index("tp")
    z_count = lax.axis_size("ep_0")
    half_width = model_width // tp_count
    head_count = half_width // LANE_WIDTH
    half_rows = own_rows // tp_count
    swap = [(0, 1), (1, 0)]

    final_row = in_row_order(row_pieces(final_projector.T, "ep_1"), "ep_1")
    qkv_rows = jnp.stack((receiver_projector.T, address_projector.T, content_projector.T))
    qkv_row = in_row_order(row_pieces(qkv_rows, "ep_1"), "ep_1")
    qkv_row = jnp.swapaxes(qkv_row, 0, 1).reshape(-1, half_width)
    final_whole = lax.all_gather(
        final_row.reshape(-1, half_width), "ep_0", axis=0, tiled=True
    )

    expert_cols = specialist_switch.shape[1]
    common_cols = common_activator.shape[1]
    pad = ((0, -common_cols % 16), (0, 0))
    block = expert_cols + common_cols + pad[0][1]
    bulk = jnp.concatenate(
        (
            specialist_switch.T,
            jnp.pad(common_activator.T, pad),
            specialist_expand.T,
            jnp.pad(common_expand.T, pad),
            specialist_contract,
            jnp.pad(common_contract, pad),
        )
    )
    bulks = row_pieces(bulk, "ep_1")

    residual = fresh_inputs.astype(F32)
    normed = rms_norm(residual, first_rescale).astype(BF16)
    normed_half = lax.dynamic_slice_in_dim(normed, tp_rank * half_width, half_width, 1)
    names = lax.broadcasted_iota(jnp.int32, (own_rows, 128), 1)
    share_table = jnp.zeros((own_rows, 128), F32)
    for k in range(chosen_specialist.shape[1]):
        share_table += jnp.where(
            chosen_specialist[:, k : k + 1] == names, chosen_coefficient[:, k : k + 1].astype(F32), 0.0
        )
    ring_own = jnp.concatenate((normed_half, share_table.astype(BF16)), axis=1)
    ring = lax.all_gather(ring_own, "ep_0", axis=0, tiled=True)
    ring_half, ring_share = ring[:, :half_width], ring[:, half_width:]

    partial = rows_dot(ring_half, qkv_row).astype(BF16)
    partial = lax.all_to_all(
        partial.reshape(z_count, own_rows, -1), "ep_0", 0, 0, tiled=True
    ).reshape(z_count, own_rows, 3, -1)
    partial = jnp.transpose(partial, (2, 1, 0, 3)).reshape(3, own_rows, model_width)
    keep = lax.dynamic_slice_in_dim(partial, tp_rank * half_width, half_width, 2)
    give = lax.dynamic_slice_in_dim(partial, (1 - tp_rank) * half_width, half_width, 2)
    got = lax.ppermute(give, "tp", swap)
    mine = (keep.astype(F32) + got.astype(F32)).astype(BF16)

    def divide_lanes(channels):
        return channels.astype(F32).reshape(own_rows, head_count, LANE_WIDTH)

    decay_mid = jnp.tanh(
        jnp.dot(normed, forget_narrowing, preferred_element_type=F32)
    ).astype(BF16)
    decay_pre = forget_bias + jnp.dot(decay_mid, forget_widening, preferred_element_type=F32)
    decay_vals = jnp.exp(-jnp.exp(-jax.nn.softplus(-decay_pre) - 0.5))
    rate_mid = jnp.dot(normed, learning_narrowing, preferred_element_type=F32).astype(BF16)
    rate_vals = jax.nn.sigmoid(
        learning_bias + jnp.dot(rate_mid, learning_widening, preferred_element_type=F32)
    )
    memory_after, memory_retrieval = evolve_memory(
        memory_arrays,
        divide_lanes(mine[0]),
        divide_lanes(mine[1]),
        divide_lanes(mine[2]),
        divide_lanes(decay_vals),
        divide_lanes(rate_vals),
        lane_scaling.reshape(head_count, LANE_WIDTH),
        instant_reward,
    )
    attended = memory_retrieval.reshape(own_rows, half_width).astype(BF16)
    out_part = rows_dot(attended, final_whole).astype(BF16)
    out_other = lax.ppermute(out_part, "tp", swap)
    mixed_out = (out_part.astype(F32) + out_other.astype(F32)).astype(BF16)
    residual = residual + mixed_out.astype(F32)
    ffn_in = rms_norm(residual, second_rescale).astype(BF16)
    own_in = lax.dynamic_slice_in_dim(ffn_in, tp_rank * half_rows, half_rows, 0)
    ring_in = lax.all_gather(own_in, "ep_0", axis=0, tiled=True)
    other_in = lax.ppermute(ring_in, "tp", swap)
    all_in = jnp.concatenate((ring_in, other_in))

    flat_rank = lax.axis_index(EP) * tp_count + tp_rank
    expert = flat_rank * expert_cols // FF_E
    ring_names = lax.broadcasted_iota(jnp.int32, ring_share.shape, 1)
    expert_share = jnp.sum(
        jnp.where(ring_names == expert, ring_share.astype(F32), 0.0), axis=1
    ).reshape(z_count, tp_count, half_rows)
    expert_share = jnp.concatenate(
        [
            lax.dynamic_slice_in_dim(expert_share, rank, 1, 1).reshape(-1)
            for rank in (tp_rank, 1 - tp_rank)
        ]
    )
    branch_scale = jax.nn.sigmoid(jnp.dot(all_in, common_switch, preferred_element_type=F32))
    columns = lax.broadcasted_iota(jnp.int32, (all_in.shape[0], block), 1)
    scale = jnp.where(columns < expert_cols, expert_share[:, None], branch_scale[:, None])
    total = None
    for piece in bulks:
        gate_val = rows_dot(all_in, piece[:block])
        up_val = rows_dot(all_in, piece[block : 2 * block])
        hidden = (jax.nn.silu(gate_val) * up_val * scale).astype(BF16)
        term = jnp.dot(hidden, piece[2 * block :], preferred_element_type=F32)
        total = term if total is None else total + term
    ring_rows = ring_in.shape[0]
    other_total = lax.ppermute(total[ring_rows:].astype(BF16), "tp", swap)
    ring_total = (total[:ring_rows] + other_total.astype(F32)).astype(BF16)
    blocks = lax.all_to_all(
        ring_total.reshape(z_count, half_rows, model_width), "ep_0", 0, 0, tiled=True
    )
    routed = jnp.sum(blocks.astype(F32), axis=0)
    own_residual = lax.dynamic_slice_in_dim(residual, tp_rank * half_rows, half_rows, 0)
    return ((own_residual + routed).astype(BF16), memory_after)


def solution(mesh):
    torus = Mesh(
        mesh.devices.reshape(mesh.shape["grp"], 16, 4, mesh.shape["tp"]),
        ("grp", "ep_0", "ep_1", "tp"),
    )
    return jax.shard_map(
        body,
        mesh=torus,
        in_specs=(
            P(GRP_EP, None),
            P(GRP_EP, "tp", None, None),
            P(GRP_EP, None),
            P(GRP_EP, None),
            P(),
            P(),
            P("tp", EP),
            P("tp", EP),
            P("tp", EP),
            P("tp", EP),
            P(),
            P(None, "tp"),
            P("tp"),
            P(),
            P(None, "tp"),
            P("tp"),
            P("tp"),
            P("tp", None),
            P(None, EP_TP),
            P(None, EP_TP),
            P(EP_TP, None),
            P(None, EP_TP),
            P(None, EP_TP),
            P(EP_TP, None),
            P(),
        ),
        out_specs=(P(GRP_EP_TP, None), P(GRP_EP, "tp", None, None)),
        check_vma=False,
    )
```

```python
import jax
import jax.numpy as jnp
from jax.experimental import pallas as pl
from jax.experimental.pallas import tpu as pltpu
from jax import lax
from jax.sharding import Mesh
from jax.sharding import PartitionSpec as P


LANE_WIDTH = 64
FF_E = 7168
EP = ("ep_0", "ep_1")
GRP_EP = ("grp", "ep_0", "ep_1")
EP_TP = ("ep_0", "ep_1", "tp")
GRP_EP_TP = ("grp", "ep_0", "ep_1", "tp")


RMS_EPS = 1e-06
GROUP_EPS = 0.00064
BF16 = jnp.bfloat16
F32 = jnp.float32


def from_ahead(value, axis, steps):
    size = lax.axis_size(axis)
    return lax.ppermute(value, axis, [((i + steps) % size, i) for i in range(size)])


def in_row_order(pieces, axis):
    count = len(pieces)
    start = (count - lax.axis_index(axis)) % count
    twice = jnp.stack(pieces + pieces[:-1])
    return lax.dynamic_slice_in_dim(twice, start, count, 0)


def rms_norm(values, norm_gain):
    mean_sq = jnp.mean(values * values, axis=-1, keepdims=True)
    return values * lax.rsqrt(mean_sq + RMS_EPS) * norm_gain


def evolve_kernel(
    memory_ref, unit_ref, erase_ref, write_ref, decay_ref, query_ref, value_ref, scaling_ref, bonus_ref,
    after_ref, attended_ref, readout_ref,
):
    heads = memory_ref.shape[1]
    for h in range(heads):
        memory = memory_ref[0, h]
        removal = jnp.sum(memory * unit_ref[0, h : h + 1, :], axis=-1, keepdims=True)
        after = (
            memory * decay_ref[0, h : h + 1, :]
            - removal * erase_ref[0, h : h + 1, :]
            + value_ref[0, :, h : h + 1] * write_ref[0, h : h + 1, :]
        )
        after_ref[0, h] = after
        readout_ref[:, h : h + 1] = jnp.sum(
            after * query_ref[0, h : h + 1, :], axis=-1, keepdims=True
        )
    readout = readout_ref[...]
    centred = readout - jnp.mean(readout, axis=0, keepdims=True)
    spread = jnp.mean(centred * centred, axis=0, keepdims=True)
    attended_ref[0] = (
        centred * lax.rsqrt(spread + GROUP_EPS) * scaling_ref[...] + bonus_ref[0] * value_ref[0]
    )


def evolve_memory(memory, query, key, value, decay, rate, scaling, reward):
    rows, heads, width, _ = memory.shape
    unit = key * lax.rsqrt(jnp.sum(key * key, axis=-1, keepdims=True) + 1.0)
    write = key * rate
    bonus = jnp.sum(query * write * reward, axis=-1)[:, None, :]
    lanes = pl.BlockSpec((1, heads, width), lambda i: (i, 0, 0))
    turned = pl.BlockSpec((1, width, heads), lambda i: (i, 0, 0))
    state = pl.BlockSpec((1, heads, width, width), lambda i: (i, 0, 0, 0))
    after, attended = pl.pallas_call(
        evolve_kernel,
        grid=(rows,),
        in_specs=[
            state, lanes, lanes, lanes, lanes, lanes, turned,
            pl.BlockSpec((width, heads), lambda i: (0, 0)),
            pl.BlockSpec((1, 1, heads), lambda i: (i, 0, 0)),
        ],
        out_specs=[state, turned],
        out_shape=[
            jax.ShapeDtypeStruct(memory.shape, F32),
            jax.ShapeDtypeStruct((rows, width, heads), F32),
        ],
        scratch_shapes=[pltpu.VMEM((width, heads), F32)],
        name="evolve",
    )(memory, unit, unit * rate, write, decay, query, jnp.swapaxes(value, 1, 2), scaling.T, bonus)
    return after, jnp.swapaxes(attended, 1, 2)


def rows_dot(left, right_rows):
    return lax.dot_general(left, right_rows, (((1,), (1,)), ((), ())), preferred_element_type=F32)


def ffn_kernel(pieces, wide, slim, own_ref, other_ref, share_ref, switch_ref, *refs):
    weights, (kept_ref, sent_ref, held, tokens, total, sems) = refs[: 4 * pieces], refs[4 * pieces :]
    block = wide + slim
    copies = []
    for p in range(pieces):
        gate, up, down, common = weights[4 * p : 4 * p + 4]
        parts = []
        for k, ref in enumerate((gate, up, down)):
            parts.append((ref, held.at[p, pl.ds(k * block, wide)]))
            parts.append((common.at[pl.ds(k * slim, slim)], held.at[p, pl.ds(k * block + wide, slim)]))
        copies.append([pltpu.make_async_copy(a, b, sems.at[p, n]) for n, (a, b) in enumerate(parts)])
    for group in copies:
        for copy in group:
            copy.start()
    half = own_ref.shape[0]
    tokens[:half] = own_ref[...]
    tokens[half:] = other_ref[...]
    every = tokens[...]
    share = share_ref[...]
    branch = jax.nn.sigmoid(rows_dot(switch_ref[...], every)[:1])
    for p in range(pieces):
        for copy in copies[p]:
            copy.wait()
        both = rows_dot(held[p, : 2 * block], every)
        gate_val, up_val = both[:block], both[block:]
        row = lax.broadcasted_iota(jnp.int32, (block, 1), 0)
        scale = jnp.where(row < wide, share, branch)
        hidden = (gate_val * jax.nn.sigmoid(gate_val) * up_val * scale).astype(BF16)
        term = lax.dot_general(
            hidden, held[p, 2 * block :], (((0,), (0,)), ((), ())), preferred_element_type=F32
        )
        if p == 0:
            total[...] = term
        elif p < pieces - 1:
            total[...] += term
        else:
            term = total[...] + term
            kept_ref[...] = term[:half]
            sent_ref[...] = term[half:].astype(BF16)


def ffn(own_in, other_in, share, switch, pieces):
    half, width = own_in.shape
    wide, slim = pieces[0][0].shape[0], pieces[0][3].shape[0] // 3
    count = len(pieces)
    vmem = pl.BlockSpec(memory_space=pltpu.VMEM)
    hbm = pl.BlockSpec(memory_space=pl.ANY)
    return pl.pallas_call(
        lambda *refs: ffn_kernel(count, wide, slim, *refs),
        in_specs=[vmem] * 4 + [hbm] * (4 * count),
        out_specs=[vmem, vmem],
        out_shape=[
            jax.ShapeDtypeStruct((half, width), F32),
            jax.ShapeDtypeStruct((half, width), BF16),
        ],
        scratch_shapes=[
            pltpu.VMEM((count, 3 * (wide + slim), width), BF16),
            pltpu.VMEM((2 * half, width), BF16),
            pltpu.VMEM((2 * half, width), F32),
            pltpu.SemaphoreType.DMA((count, 6)),
        ],
        compiler_params=pltpu.CompilerParams(vmem_limit_bytes=48 * 1024 * 1024),
        name="ffn",
    )(own_in, other_in, share, switch, *[ref for piece in pieces for ref in piece])


def body(
    fresh_inputs,
    memory_arrays,
    chosen_specialist,
    chosen_coefficient,
    first_rescale,
    second_rescale,
    receiver_projector,
    address_projector,
    content_projector,
    final_projector,
    forget_narrowing,
    forget_widening,
    forget_bias,
    learning_narrowing,
    learning_widening,
    learning_bias,
    lane_scaling,
    instant_reward,
    specialist_switch,
    specialist_expand,
    specialist_contract,
    common_activator,
    common_expand,
    common_contract,
    common_switch,
):
    own_rows, model_width = fresh_inputs.shape
    tp_count = lax.axis_size("tp")
    tp_rank = lax.axis_index("tp")
    z_count = lax.axis_size("ep_0")
    x_count = lax.axis_size("ep_1")
    half_width = model_width // tp_count
    head_count = half_width // LANE_WIDTH
    half_rows = own_rows // tp_count
    swap = [(0, 1), (1, 0)]

    def pick(value, rank, width, dim):
        return lax.dynamic_slice_in_dim(value, rank * width, width, dim)

    projector_rows = jnp.stack(
        (receiver_projector.T, address_projector.T, content_projector.T, final_projector.T)
    )
    projector_row = in_row_order(
        [projector_rows] + [from_ahead(projector_rows, "ep_1", k) for k in range(1, x_count)], "ep_1"
    )
    qkv_row = jnp.swapaxes(projector_row[:, :3], 0, 1).reshape(-1, half_width)
    final_row = projector_row[:, 3].reshape(-1, half_width)

    expert_cols = specialist_switch.shape[1]
    pad = ((0, -common_activator.shape[1] % 16), (0, 0))
    common = jnp.concatenate(
        [jnp.pad(w, pad) for w in (common_activator.T, common_expand.T, common_contract)]
    )
    own_piece = [specialist_switch.T, specialist_expand.T, specialist_contract, common]
    ahead, behind, across = [], [], []
    for w in own_piece:
        ahead.append(from_ahead(w, "ep_1", 1))
        behind.append(from_ahead(w, "ep_1", x_count - 1))
    for k in range(len(own_piece)):
        if k % 2 == 0:
            across.append(from_ahead(ahead[k], "ep_1", 1))
        else:
            across.append(from_ahead(behind[k], "ep_1", x_count - 1))
    pieces = [own_piece, ahead, behind, across]

    names = lax.broadcasted_iota(jnp.int32, (own_rows, 128), 1)
    share_table = jnp.zeros((own_rows, 128), F32)
    for k in range(chosen_specialist.shape[1]):
        share_table += jnp.where(
            chosen_specialist[:, k : k + 1] == names, chosen_coefficient[:, k : k + 1].astype(F32), 0.0
        )
    ring_own = jnp.concatenate((fresh_inputs, share_table.astype(BF16)), axis=1)
    ring_own = pick(ring_own, tp_rank, half_rows, 0)
    ring = lax.all_gather(ring_own, "ep_0", axis=0, tiled=True)
    ring_rows = ring.shape[0]
    ring_share = ring[:, model_width:]
    ring_fresh = ring[:, :model_width].astype(F32)
    ring_normed = rms_norm(ring_fresh, first_rescale).astype(BF16)
    give = jnp.concatenate((pick(ring_normed, 1 - tp_rank, half_width, 1), ring_share), axis=1)
    got = lax.ppermute(give, "tp", swap)
    other_share = got[:, half_width:]
    mine = pick(ring_normed, tp_rank, half_width, 1).reshape(z_count, 1, half_rows, half_width)
    theirs = got[:, :half_width].reshape(z_count, 1, half_rows, half_width)
    first = tp_rank == 0
    ring_half = jnp.concatenate(
        (jnp.where(first, mine, theirs), jnp.where(first, theirs, mine)), axis=1
    ).reshape(z_count * own_rows, half_width)

    partial = rows_dot(ring_half, qkv_row).astype(BF16)
    partial = lax.all_to_all(
        partial.reshape(z_count, own_rows, -1), "ep_0", 0, 0, tiled=True
    ).reshape(z_count, own_rows, 3, -1)
    partial = jnp.transpose(partial, (2, 1, 0, 3)).reshape(3, own_rows, model_width)
    got = lax.ppermute(pick(partial, 1 - tp_rank, half_width, 2), "tp", swap)
    projected = (pick(partial, tp_rank, half_width, 2).astype(F32) + got.astype(F32)).astype(BF16)

    def divide_lanes(channels):
        return channels.astype(F32).reshape(own_rows, head_count, LANE_WIDTH)

    normed = rms_norm(fresh_inputs.astype(F32), first_rescale).astype(BF16)
    decay_mid = jnp.tanh(
        jnp.dot(normed, forget_narrowing, preferred_element_type=F32)
    ).astype(BF16)
    decay_pre = forget_bias + jnp.dot(decay_mid, forget_widening, preferred_element_type=F32)
    decay_vals = jnp.exp(-jnp.exp(-jax.nn.softplus(-decay_pre) - 0.5))
    rate_mid = jnp.dot(normed, learning_narrowing, preferred_element_type=F32).astype(BF16)
    rate_vals = jax.nn.sigmoid(
        learning_bias + jnp.dot(rate_mid, learning_widening, preferred_element_type=F32)
    )
    memory_after, memory_retrieval = evolve_memory(
        memory_arrays,
        divide_lanes(projected[0]),
        divide_lanes(projected[1]),
        divide_lanes(projected[2]),
        divide_lanes(decay_vals),
        divide_lanes(rate_vals),
        lane_scaling.reshape(head_count, LANE_WIDTH),
        instant_reward,
    )
    attended = memory_retrieval.reshape(own_rows, half_width).astype(BF16)
    ring_attended = lax.all_gather(attended, "ep_0", axis=0, tiled=True)
    out_part = rows_dot(ring_attended, final_row).astype(BF16)
    out_part = out_part.reshape(z_count, own_rows, -1)
    got = lax.ppermute(pick(out_part, 1 - tp_rank, half_rows, 1), "tp", swap)
    mixed = (pick(out_part, tp_rank, half_rows, 1).astype(F32) + got.astype(F32)).astype(BF16)
    mixed = mixed.reshape(1, ring_rows, -1)
    mixed = lax.all_gather(mixed, "ep_0", axis=0, tiled=True)
    mixed = jnp.swapaxes(mixed, 0, 1).reshape(ring_rows, model_width)
    residual = ring_fresh + mixed.astype(F32)
    ring_in = rms_norm(residual, second_rescale).astype(BF16)
    other_in = lax.ppermute(ring_in, "tp", swap)

    flat_rank = lax.axis_index(EP) * tp_count + tp_rank
    expert = flat_rank * expert_cols // FF_E
    share = jnp.concatenate((ring_share, other_share)).astype(F32)
    lane = lax.broadcasted_iota(jnp.int32, share.shape, 1)
    expert_share = jnp.sum(jnp.where(lane == expert, share, 0.0), axis=1)[None, :]
    switch = jnp.broadcast_to(common_switch[None, :], (16, model_width))
    kept, sent = ffn(ring_in, other_in, expert_share, switch, pieces)
    got = lax.ppermute(sent, "tp", swap)
    ring_total = (kept + got.astype(F32)).astype(BF16)
    blocks = lax.all_to_all(
        ring_total.reshape(z_count, half_rows, model_width), "ep_0", 0, 0, tiled=True
    )
    routed = jnp.sum(blocks.astype(F32), axis=0)
    own_residual = pick(residual, lax.axis_index("ep_0"), half_rows, 0)
    return ((own_residual + routed).astype(BF16), memory_after)


def solution(mesh):
    torus = Mesh(
        mesh.devices.reshape(mesh.shape["grp"], 16, 4, mesh.shape["tp"]),
        ("grp", "ep_0", "ep_1", "tp"),
    )
    return jax.shard_map(
        body,
        mesh=torus,
        in_specs=(
            P(GRP_EP, None),
            P(GRP_EP, "tp", None, None),
            P(GRP_EP, None),
            P(GRP_EP, None),
            P(),
            P(),
            P("tp", EP),
            P("tp", EP),
            P("tp", EP),
            P("tp", EP),
            P(),
            P(None, "tp"),
            P("tp"),
            P(),
            P(None, "tp"),
            P("tp"),
            P("tp"),
            P("tp", None),
            P(None, EP_TP),
            P(None, EP_TP),
            P(EP_TP, None),
            P(None, EP_TP),
            P(None, EP_TP),
            P(EP_TP, None),
            P(),
        ),
        out_specs=(P(GRP_EP_TP, None), P(GRP_EP, "tp", None, None)),
        check_vma=False,
    )
```

```python
import jax
import jax.numpy as jnp
from jax.experimental import pallas as pl
from jax.experimental.pallas import tpu as pltpu
from jax import lax
from jax.sharding import Mesh
from jax.sharding import PartitionSpec as P


LANE_WIDTH = 64
FF_E = 7168
Z = ("ep_0", "ep_1")
X = "ep_2"
EP = ("ep_0", "ep_1", "ep_2")
GRP_EP = ("grp", *EP)
EP_TP = (*EP, "tp")
GRP_EP_TP = ("grp", *EP, "tp")
NEAR = (-1, 0, 1, 2)


RMS_EPS = 1e-06
GROUP_EPS = 0.00064
BF16 = jnp.bfloat16
F32 = jnp.float32


def from_ahead(value, axis, steps):
    size = lax.axis_size(axis)
    return lax.ppermute(value, axis, [((i + steps) % size, i) for i in range(size)])


def turned_lanes(width, x_count, x_rank):
    block = width // x_count
    rows = lax.broadcasted_iota(jnp.int32, (width, width), 0)
    columns = lax.broadcasted_iota(jnp.int32, (width, width), 1)
    moved = rows + x_rank * block
    return (jnp.where(moved >= width, moved - width, moved) == columns).astype(BF16)


def rms_norm(values, norm_gain):
    mean_sq = jnp.mean(values * values, axis=-1, keepdims=True)
    return values * lax.rsqrt(mean_sq + RMS_EPS) * norm_gain


def rows_dot(left, right_rows):
    return lax.dot_general(left, right_rows, (((1,), (1,)), ((), ())), preferred_element_type=F32)


def evolve_kernel(
    memory_ref, query_ref, key_ref, value_ref, decay_ref, rate_ref, scaling_ref, reward_ref,
    after_ref, attended_ref, readout_ref,
):
    rows, heads, width, _ = memory_ref.shape
    eye = (
        lax.broadcasted_iota(jnp.int32, (width, width), 0)
        == lax.broadcasted_iota(jnp.int32, (width, width), 1)
    ).astype(F32).astype(BF16)

    def one_row(r, carry):
        query, key, value = query_ref[r], key_ref[r], value_ref[r]
        decay, rate = decay_ref[r], rate_ref[r]
        unit = key * lax.rsqrt(jnp.sum(key * key, axis=-1, keepdims=True) + 1.0)
        erase = unit * rate
        write = key * rate
        for h in range(heads):
            memory = memory_ref[r, h]
            removal = jnp.sum(memory * unit[h : h + 1], axis=-1, keepdims=True)
            spread_value = jnp.broadcast_to(value[h : h + 1], (width, width)).astype(BF16)
            after = (
                memory * decay[h : h + 1]
                - removal * erase[h : h + 1]
                + rows_dot(eye, spread_value) * write[h : h + 1]
            )
            after_ref[r, h] = after
            high = after.astype(BF16)
            low = (after - high.astype(F32)).astype(BF16)
            wanted = jnp.broadcast_to(query[h : h + 1], (16, width)).astype(BF16)
            readout_ref[h : h + 1] = (rows_dot(wanted, high) + rows_dot(wanted, low))[:1]
        readout = readout_ref[...]
        centred = readout - jnp.mean(readout, axis=-1, keepdims=True)
        variance = jnp.mean(centred * centred, axis=-1, keepdims=True)
        bonus = jnp.sum(query * write * reward_ref[...], axis=-1, keepdims=True)
        attended_ref[r] = (
            centred * lax.rsqrt(variance + GROUP_EPS) * scaling_ref[...] + bonus * value
        ).astype(BF16)
        return carry

    lax.fori_loop(0, rows, one_row, 0)


def evolve_memory(memory, query, key, value, decay, rate, scaling, reward):
    rows, heads, width, _ = memory.shape
    step = rows // 4
    lanes = pl.BlockSpec((step, heads, width), lambda i: (i, 0, 0))
    fixed = pl.BlockSpec((heads, width), lambda i: (0, 0))
    state = pl.BlockSpec((step, heads, width, width), lambda i: (i, 0, 0, 0))
    return pl.pallas_call(
        evolve_kernel,
        grid=(rows // step,),
        in_specs=[state] + [lanes] * 5 + [fixed] * 2,
        out_specs=[state, lanes],
        out_shape=[
            jax.ShapeDtypeStruct(memory.shape, F32),
            jax.ShapeDtypeStruct((rows, heads, width), BF16),
        ],
        scratch_shapes=[pltpu.VMEM((heads, width), F32)],
        name="evolve",
    )(memory, query, key, value, decay, rate, scaling, reward)


def ffn_kernel(pieces, wide, slim, own_ref, other_ref, share_ref, switch_ref, *refs):
    weights, (kept_ref, sent_ref, held, tokens, total, sems) = refs[: 4 * pieces], refs[4 * pieces :]
    block = wide + slim
    copies = []
    for p in range(pieces):
        gate, up, down, common = weights[4 * p : 4 * p + 4]
        parts = []
        for k, ref in enumerate((gate, up, down)):
            parts.append((ref, held.at[p, pl.ds(k * block, wide)]))
            parts.append((common.at[pl.ds(k * slim, slim)], held.at[p, pl.ds(k * block + wide, slim)]))
        copies.append([pltpu.make_async_copy(a, b, sems.at[p, n]) for n, (a, b) in enumerate(parts)])
    for group in copies:
        for copy in group:
            copy.start()
    half = own_ref.shape[0]
    width = tokens.shape[1]
    tokens[:half] = own_ref[:, :width]
    tokens[half:] = other_ref[:, :width]
    every = tokens[...]
    share = share_ref[...]
    branch = jax.nn.sigmoid(rows_dot(switch_ref[...], every)[:1])
    for p in range(pieces):
        for copy in copies[p]:
            copy.wait()
        both = rows_dot(held[p, : 2 * block], every)
        gate_val, up_val = both[:block], both[block:]
        row = lax.broadcasted_iota(jnp.int32, (block, 1), 0)
        scale = jnp.where(row < wide, share, branch)
        hidden = (gate_val * jax.nn.sigmoid(gate_val) * up_val * scale).astype(BF16)
        term = lax.dot_general(
            hidden, held[p, 2 * block :], (((0,), (0,)), ((), ())), preferred_element_type=F32
        )
        if p == 0:
            total[...] = term
        elif p < pieces - 1:
            total[...] += term
        else:
            term = total[...] + term
            kept_ref[...] = term[:half]
            sent_ref[...] = term[half:].astype(BF16)


def ffn(own_in, other_in, share, switch, pieces):
    half, width = own_in.shape[0], switch.shape[1]
    wide, slim = pieces[0][0].shape[0], pieces[0][3].shape[0] // 3
    count = len(pieces)
    vmem = pl.BlockSpec(memory_space=pltpu.VMEM)
    hbm = pl.BlockSpec(memory_space=pl.ANY)
    return pl.pallas_call(
        lambda *refs: ffn_kernel(count, wide, slim, *refs),
        in_specs=[vmem] * 4 + [hbm] * (4 * count),
        out_specs=[vmem, vmem],
        out_shape=[
            jax.ShapeDtypeStruct((half, width), F32),
            jax.ShapeDtypeStruct((half, width), BF16),
        ],
        scratch_shapes=[
            pltpu.VMEM((count, 3 * (wide + slim), width), BF16),
            pltpu.VMEM((2 * half, width), BF16),
            pltpu.VMEM((2 * half, width), F32),
            pltpu.SemaphoreType.DMA((count, 6)),
        ],
        compiler_params=pltpu.CompilerParams(vmem_limit_bytes=48 * 1024 * 1024),
        name="ffn",
    )(own_in, other_in, share, switch, *[ref for piece in pieces for ref in piece])


def body(
    fresh_inputs,
    memory_arrays,
    chosen_specialist,
    chosen_coefficient,
    first_rescale,
    second_rescale,
    receiver_projector,
    address_projector,
    content_projector,
    final_projector,
    forget_narrowing,
    forget_widening,
    forget_bias,
    learning_narrowing,
    learning_widening,
    learning_bias,
    lane_scaling,
    instant_reward,
    specialist_switch,
    specialist_expand,
    specialist_contract,
    common_activator,
    common_expand,
    common_contract,
    common_switch,
):
    own_rows, model_width = fresh_inputs.shape
    tp_count = lax.axis_size("tp")
    tp_rank = lax.axis_index("tp")
    z_count = lax.axis_size(Z)
    x_rank, x_count = lax.axis_index(X), lax.axis_size(X)
    far_count, near_rank = lax.axis_size("ep_0"), lax.axis_index("ep_1")
    half_width = model_width // tp_count
    head_count = half_width // LANE_WIDTH
    half_rows = own_rows // tp_count
    swap = [(0, 1), (1, 0)]

    def pick(value, rank, width, dim):
        return lax.dynamic_slice_in_dim(value, rank * width, width, dim)

    def ring_piece(value, steps):
        return value if steps == 0 else from_ahead(value, Z, steps % z_count)

    def row_piece(value, steps):
        return value if steps == 0 else from_ahead(value, X, steps)

    qkv_rows = jnp.stack(
        (receiver_projector.T, address_projector.T, content_projector.T)
    )
    lane_cols = receiver_projector.shape[1]
    qkv_pieces = [row_piece(qkv_rows, k) for k in range(x_count)]
    expert_cols = specialist_switch.shape[1]
    pad = ((0, -common_activator.shape[1] % 16), (0, 0))
    common = jnp.concatenate(
        [jnp.pad(w, pad) for w in (common_activator.T, common_expand.T, common_contract)]
    )
    own_piece = [specialist_switch.T, specialist_expand.T, specialist_contract, common]
    final_rows = jnp.stack([ring_piece(final_projector.T, k) for k in NEAR])
    final_pieces = [row_piece(final_rows, k) for k in range(x_count)]
    ahead, behind, across = [], [], []
    for w in own_piece:
        ahead.append(from_ahead(w, X, 1))
        behind.append(from_ahead(w, X, x_count - 1))
    for k in range(len(own_piece)):
        if k % 2 == 0:
            across.append(from_ahead(ahead[k], X, 1))
        else:
            across.append(from_ahead(behind[k], X, x_count - 1))
    pieces = [own_piece, ahead, behind, across]

    ring = lax.all_gather(
        pick(fresh_inputs, tp_rank, half_rows, 0), Z, axis=0, tiled=True
    )
    ring_fresh = ring.astype(F32)
    ring_normed = rms_norm(ring_fresh, first_rescale).astype(BF16)
    got = lax.ppermute(pick(ring_normed, 1 - tp_rank, half_width, 1), "tp", swap)
    mine = pick(ring_normed, tp_rank, half_width, 1).reshape(z_count, 1, half_rows, half_width)
    theirs = got.reshape(z_count, 1, half_rows, half_width)
    first = tp_rank == 0
    ring_half = jnp.concatenate(
        (jnp.where(first, mine, theirs), jnp.where(first, theirs, mine)), axis=1
    ).reshape(z_count * own_rows, half_width)

    qkv_row = jnp.concatenate(qkv_pieces, axis=1).reshape(-1, half_width)
    partial = rows_dot(ring_half, qkv_row).astype(BF16)
    partial = lax.all_to_all(
        partial.reshape(z_count, own_rows, -1), Z, 0, 0, tiled=True
    )
    turn = turned_lanes(x_count * lane_cols, x_count, x_rank)
    partial = jnp.transpose(partial.reshape(z_count, own_rows, 3, -1), (2, 1, 0, 3))
    partial = jnp.dot(partial, turn, preferred_element_type=F32).astype(BF16)
    partial = partial.reshape(3, own_rows, model_width)
    got = lax.ppermute(pick(partial, 1 - tp_rank, half_width, 2), "tp", swap)
    projected = (pick(partial, tp_rank, half_width, 2).astype(F32) + got.astype(F32)).astype(BF16)

    def divide_lanes(channels):
        return channels.astype(F32).reshape(own_rows, head_count, LANE_WIDTH)

    normed = rms_norm(fresh_inputs.astype(F32), first_rescale).astype(BF16)
    decay_mid = jnp.tanh(
        jnp.dot(normed, forget_narrowing, preferred_element_type=F32)
    ).astype(BF16)
    decay_pre = forget_bias + jnp.dot(decay_mid, forget_widening, preferred_element_type=F32)
    decay_vals = jnp.exp(-jnp.exp(-jax.nn.softplus(-decay_pre) - 0.5))
    rate_mid = jnp.dot(normed, learning_narrowing, preferred_element_type=F32).astype(BF16)
    rate_vals = jax.nn.sigmoid(
        learning_bias + jnp.dot(rate_mid, learning_widening, preferred_element_type=F32)
    )
    memory_after, attended = evolve_memory(
        memory_arrays,
        divide_lanes(projected[0]),
        divide_lanes(projected[1]),
        divide_lanes(projected[2]),
        divide_lanes(decay_vals),
        divide_lanes(rate_vals),
        lane_scaling.reshape(head_count, LANE_WIDTH),
        instant_reward,
    )

    names = lax.broadcasted_iota(jnp.int32, (own_rows, 128), 1)
    share_table = jnp.zeros((own_rows, 128), F32)
    for k in range(chosen_specialist.shape[1]):
        share_table += jnp.where(
            chosen_specialist[:, k : k + 1] == names, chosen_coefficient[:, k : k + 1].astype(F32), 0.0
        )
    attended = jnp.concatenate(
        (attended.reshape(own_rows, half_width), share_table.astype(BF16)), axis=1
    )
    far = lax.all_gather(attended, "ep_0", axis=0, tiled=True)
    far_share = pick(far[:, half_width:].reshape(far_count, own_rows, -1), tp_rank, half_rows, 1)
    final_row = jnp.concatenate(final_pieces, axis=1).reshape(-1, half_width)
    far_part = rows_dot(far[:, :half_width], final_row).astype(BF16)
    far_part = far_part.reshape(far_count, own_rows, -1)
    got = lax.ppermute(pick(far_part, 1 - tp_rank, half_rows, 1), "tp", swap)
    far_rows = far_count * half_rows
    mixed = (pick(far_part, tp_rank, half_rows, 1).astype(F32) + got.astype(F32)).astype(BF16)
    mixed = mixed.reshape(far_rows, -1)
    mixed = lax.all_gather(mixed[None], "ep_0", axis=0, tiled=True)
    mixed = jnp.swapaxes(mixed.reshape(far_count, far_rows, len(NEAR), -1), 1, 2)
    mixed = mixed.reshape(z_count, far_rows, -1)
    mixed = lax.dynamic_slice_in_dim(
        jnp.concatenate((mixed, mixed)), (z_count - NEAR[0] - near_rank) % z_count, z_count, 0
    )
    mixed = jnp.dot(mixed, turn, preferred_element_type=F32).astype(BF16)
    mixed = jnp.swapaxes(mixed, 0, 1).reshape(far_rows, model_width)
    far_fresh = pick(
        ring_fresh.reshape(far_count, len(NEAR), half_rows, model_width), near_rank, 1, 1
    ).reshape(far_rows, model_width)
    residual = far_fresh + mixed.astype(F32)
    far_in = rms_norm(residual, second_rescale).astype(BF16)
    far_in = jnp.concatenate((far_in, far_share.reshape(far_rows, -1)), axis=1)
    own_in = jnp.concatenate([ring_piece(far_in, k) for k in NEAR])
    other_in = lax.ppermute(own_in, "tp", swap)

    flat_rank = lax.axis_index(EP) * tp_count + tp_rank
    expert = flat_rank * expert_cols // FF_E
    share = jnp.concatenate((own_in[:, model_width:], other_in[:, model_width:])).astype(F32)
    lane = lax.broadcasted_iota(jnp.int32, share.shape, 1)
    expert_share = jnp.sum(jnp.where(lane == expert, share, 0.0), axis=1)[None, :]
    switch = jnp.broadcast_to(common_switch[None, :], (16, model_width))
    kept, sent = ffn(own_in, other_in, expert_share, switch, pieces)
    got = lax.ppermute(sent, "tp", swap)
    near_total = (kept + got.astype(F32)).astype(BF16).reshape(len(NEAR), far_rows, model_width)
    far_total = sum(
        ring_piece(near_total[n], -k).astype(F32) for n, k in enumerate(NEAR)
    ).astype(BF16)
    blocks = lax.all_to_all(
        far_total.reshape(far_count, half_rows, model_width), "ep_0", 0, 0, tiled=True
    )
    routed = jnp.sum(blocks.astype(F32), axis=0)
    own_residual = pick(residual, lax.axis_index("ep_0"), half_rows, 0)
    return ((own_residual + routed).astype(BF16), memory_after)


def solution(mesh):
    torus = Mesh(
        mesh.devices.reshape(mesh.shape["grp"], 4, 4, 4, mesh.shape["tp"]),
        ("grp", *EP, "tp"),
    )
    return jax.shard_map(
        body,
        mesh=torus,
        in_specs=(
            P(GRP_EP, None),
            P(GRP_EP, "tp", None, None),
            P(GRP_EP, None),
            P(GRP_EP, None),
            P(),
            P(),
            P("tp", EP),
            P("tp", EP),
            P("tp", EP),
            P("tp", EP),
            P(),
            P(None, "tp"),
            P("tp"),
            P(),
            P(None, "tp"),
            P("tp"),
            P("tp"),
            P("tp", None),
            P(None, EP_TP),
            P(None, EP_TP),
            P(EP_TP, None),
            P(None, EP_TP),
            P(None, EP_TP),
            P(EP_TP, None),
            P(),
        ),
        out_specs=(P(GRP_EP_TP, None), P(GRP_EP, "tp", None, None)),
        check_vma=False,
    )
```
